32 devices in a mesh: sp: 8 (over z, y), tp: 4 (over x, core).
Axes of the slice: x: 2, y: 2, z: 4, core: 2. Of those that a mesh axis runs over, the one named last changes fastest.
Arguments:
- residual: bfloat16 [2048, 2048], P('sp'), may hold values from -6 to 6
- queries: bfloat16 [2048, 8, 2, 128], P('sp', 'tp'), may hold values from -100 to 100
- key_rows: bfloat16 [2048, 8, 2, 128], P('sp', 'tp'), may hold values from -6 to 6
- values: bfloat16 [2048, 8, 256], P('sp', 'tp'), may hold values from -6 to 6
- lambda_head: float32 [8], P('tp'), may hold values from 0.3 to 0.8
- sub_gain: float32 [256], replicated, may hold values from 0.1 to 1.9
- w_out: bfloat16 [2048, 2048], P('tp'), may hold values from -0.125 to 0.125
- norm_gain: float32 [2048], replicated, may hold values from 0.1 to 1.9
- w_gate: bfloat16 [2048, 5632], P('sp', 'tp'), may hold values from -0.125 to 0.125
- w_up: bfloat16 [2048, 5632], P('sp', 'tp'), may hold values from -0.125 to 0.125
- conv_gate: float32 [3, 5632], P(None, 'tp'), may hold values from -3 to 3
- conv_up: float32 [3, 5632], P(None, 'tp'), may hold values from -3 to 3
- w_down: bfloat16 [5632, 2048], P('tp'), may hold values from -0.078125 to 0.078125
Outputs:
- layer_out: bfloat16 [2048, 2048], P(('sp', 'tp'))
The draws below stay inside these ranges and needn't reach their ends.
All inputs are finite; a program needn't handle non-finite values.
Results may differ from the reference program's by a relative error of at most 0.017.
Values may be sent and summed in bfloat16 or wider, within the bound.
A program may use at most 192 MiB of HBM per device.

```python
import math
import jax
import jax.numpy as jnp
from jax import lax

D = 2048
HEADS = 8
DH = 128
DV = 256
FF = 5632
TOKENS = 2048


def query_key_pair(key):
    shape = (TOKENS, HEADS, 2, DH)
    keys_drawn = jnp.clip(1.3 * jax.random.normal(jax.random.fold_in(key, 12), shape, jnp.float32), -6.0, 6.0)
    queries_drawn = jnp.clip(1.3 * jax.random.normal(jax.random.fold_in(key, 11), shape, jnp.float32), -6.0, 6.0)
    return (queries_drawn, keys_drawn)


def draw_queries(key, part):
    return query_key_pair(key)[0].astype(jnp.bfloat16)


def draw_key_rows(key, part):
    return query_key_pair(key)[1].astype(jnp.bfloat16)


def block_scale(stream_key, extent, pieces, low, largest):
    def one(dim, shards_of):
        steps = jax.random.uniform(jax.random.fold_in(jax.random.fold_in(stream_key, 6), dim), (shards_of,), jnp.float32, low / len(pieces), largest / len(pieces))
        return jnp.repeat(jnp.exp(steps), extent[dim] // shards_of).reshape((-1,) + (1,) * (len(extent) - dim - 1))

    level = one(*pieces[0])
    for cut in pieces[1:]:
        level = level * one(*cut)
    return level


def normal_values(stream_key, dims, width, reach, split=(), held_as=jnp.bfloat16):
    result = width * jax.random.normal(stream_key, dims, jnp.float32)
    if split:
        result = result * block_scale(stream_key, dims, split, -0.22, 0.18)
    return jnp.clip(result, -reach, reach).astype(held_as)


def setup_inputs(seed: int = 0) -> dict:
    seeds = jax.random.split(jax.random.key(seed), 14)
    return {
        "residual": normal_values(seeds[0], (TOKENS, D), 1.0, 6.0, ((0, 8),)),
        "queries": draw_queries(jax.random.fold_in(seeds[13], 71), 0),
        "key_rows": draw_key_rows(jax.random.fold_in(seeds[13], 71), 0),
        "values": normal_values(seeds[3], (TOKENS, HEADS, DV), 1.0, 6.0, ((0, 8), (1, 4))),
        "lambda_head": jnp.clip(0.3 + 0.5 * jax.random.uniform(seeds[4], (HEADS,), jnp.float32) ** block_scale(seeds[4], (HEADS,), ((0, 4),), -0.2, 0.2), 0.3, 0.8),
        "sub_gain": jnp.clip(1.0 + 0.18 * jax.random.normal(seeds[5], (DV,), jnp.float32), 0.1, 1.9),
        "w_out": normal_values(seeds[6], (HEADS * DV, D), (HEADS * DV) ** -0.5, 0.125, ((0, 4),)),
        "norm_gain": jnp.clip(1.0 + 0.18 * jax.random.normal(seeds[7], (D,), jnp.float32), 0.1, 1.9),
        "w_gate": normal_values(seeds[8], (D, FF), D ** -0.5, 0.125, ((0, 8), (1, 4))),
        "w_up": normal_values(seeds[9], (D, FF), D ** -0.5, 0.125, ((0, 8), (1, 4))),
        "conv_gate": normal_values(seeds[10], (3, FF), 0.577, 3.0, ((1, 4),), jnp.float32),
        "conv_up": normal_values(seeds[11], (3, FF), 0.577, 3.0, ((1, 4),), jnp.float32),
        "w_down": normal_values(seeds[12], (FF, D), FF ** -0.5, 0.078125, ((0, 4),)),
    }


epsilon = 1e-06
lambda_init = 0.8 - 0.6 * math.exp(-0.3)

def causal_mix(rows_in, taps):
    padded_rows = jnp.concatenate([jnp.zeros((2, rows_in.shape[1]), jnp.float32), rows_in.astype(jnp.float32)], 0)
    return taps[0] * padded_rows[:-2] + taps[1] * padded_rows[1:-1] + taps[2] * padded_rows[2:]

def reference(residual, queries, key_rows, values, lambda_head, sub_gain, w_out, norm_gain, w_gate, w_up, conv_gate, conv_up, w_down):
    query_block = math.gcd(TOKENS, 256)
    score_scale = 1.0 / math.sqrt(DH)
    key_pos = jnp.arange(TOKENS, dtype=jnp.int32)
    keys_wide = key_rows.astype(jnp.float32)
    values_wide = values.astype(jnp.float32)

    def attend(block_start):
        query_part = lax.dynamic_slice_in_dim(queries, block_start, query_block, 0).astype(jnp.float32)
        scores = jnp.einsum('qhcd,khcd->hcqk', query_part, keys_wide) * score_scale
        query_pos = block_start + jnp.arange(query_block, dtype=jnp.int32)
        causal_mask = key_pos[None, :] <= query_pos[:, None]
        scores = jnp.where(causal_mask, scores, -1e+30)
        run_max = lax.optimization_barrier(jnp.max(scores, axis=-1, keepdims=True))
        weights = jnp.where(causal_mask, jnp.exp(scores - run_max), 0.0)
        run_sum = lax.optimization_barrier(jnp.sum(weights, axis=-1))
        rounded = lax.optimization_barrier(weights.astype(jnp.bfloat16)).astype(jnp.float32)
        summed = jnp.einsum('hcqk,khe->hcqe', rounded, values_wide)
        blended = summed / run_sum[..., None]
        return blended[:, 0] - lambda_head[:, None, None] * blended[:, 1]
    starts = (jnp.arange(TOKENS // query_block, dtype=jnp.int32) * query_block).astype(jnp.int32)
    attended = lax.map(attend, starts)
    attended = jnp.transpose(attended, (0, 2, 1, 3)).reshape(TOKENS, HEADS, DV)
    mean_square = lax.optimization_barrier(jnp.mean(attended * attended, axis=-1, keepdims=True))
    normed = attended * lax.rsqrt(mean_square + epsilon) * sub_gain * (1.0 - lambda_init)
    normed = normed.astype(jnp.bfloat16).reshape(TOKENS, HEADS * DV)
    middle = residual.astype(jnp.float32) + jnp.dot(normed, w_out, preferred_element_type=jnp.float32)
    row_square = lax.optimization_barrier(jnp.mean(middle * middle, axis=-1, keepdims=True))
    normed_rows = (middle * lax.rsqrt(row_square + epsilon) * norm_gain).astype(jnp.bfloat16)
    gate_pre = jnp.dot(normed_rows, w_gate, preferred_element_type=jnp.float32).astype(jnp.bfloat16)
    up_pre = jnp.dot(normed_rows, w_up, preferred_element_type=jnp.float32).astype(jnp.bfloat16)
    gate_mixed = causal_mix(gate_pre, conv_gate)
    up_mixed = causal_mix(up_pre, conv_up)
    hidden = (jax.nn.silu(gate_mixed) * up_mixed).astype(jnp.bfloat16)
    lowered = jnp.dot(hidden, w_down, preferred_element_type=jnp.float32)
    return (middle + lowered).astype(jnp.bfloat16)
```

```python
import functools
import math

import jax
import jax.numpy as jnp
from jax import lax
from jax.experimental import pallas as pl
from jax.experimental.pallas import tpu as pltpu
from jax.sharding import PartitionSpec as P

MESH = pl.DeviceIdType.MESH
epsilon = 1e-06
lambda_init = 0.8 - 0.6 * math.exp(-0.3)
bf16 = jnp.bfloat16
f32 = jnp.float32
HALO = 16
UP, DOWN, ACROSS = 0, 1, 2
KV, GATE, UP_A, UP_B = 0, 1, 2, 3


def kernel(
    S, T, heads, dh, dv,
    q_hbm, kv_hbm, res_hbm, wout_hbm, wg_hbm, wu_hbm, wd_hbm,
    lam_ref, sub_ref, norm_ref, cg_ref, cu_ref,
    out_ref,
    q, kv, res, wout, wg, wua, wub, wd,
    m_s, l_s, acc_s, n_s, part, part_in, mid, hn, hb, halo_in, acc_g, acc_u, hid, low, low_in,
    local_sem, send_sem, recv_sem, tp_send, tp_recv, halo_sem, low_send, low_recv,
):
    Z = S // 2
    sp = lax.axis_index("sp")
    tp = lax.axis_index("tp")
    z = lax.div(sp, 2)
    y = lax.rem(sp, 2)
    rows = q.shape[0]
    feat = wg.shape[1]
    half = feat // 2
    D = wout.shape[1]
    own = rows // T
    units = wg.shape[2]
    has_up, has_down = z < Z - 1, z > 0
    has_next, has_prev = sp < S - 1, sp > 0

    def one(flag):
        return flag.astype(jnp.int32)

    def peer(d):
        return lax.rem(tp + d, T)

    target = {UP: sp + 2, DOWN: sp - 2, ACROSS: z * 2 + (1 - y)}
    bufs = {KV: kv, GATE: wg, UP_A: wua, UP_B: wub}

    loads = [
        pltpu.make_async_copy(kv_hbm, kv.at[sp], local_sem.at[0]),
        pltpu.make_async_copy(wg_hbm, wg.at[sp], local_sem.at[1]),
        pltpu.make_async_copy(wu_hbm.at[pl.ds(0, half)], wua.at[sp], local_sem.at[2]),
        pltpu.make_async_copy(wu_hbm.at[pl.ds(half, half)], wub.at[sp], local_sem.at[3]),
        pltpu.make_async_copy(q_hbm, q, local_sem.at[4]),
        pltpu.make_async_copy(wout_hbm, wout, local_sem.at[5]),
        pltpu.make_async_copy(res_hbm, res, local_sem.at[6]),
        pltpu.make_async_copy(wd_hbm, wd, local_sem.at[7]),
    ]
    for c in loads:
        c.start()

    barrier = pltpu.get_barrier_semaphore()

    def greet(device):
        pl.semaphore_signal(barrier, inc=1, device_id=device, device_id_type=MESH)

    pl.when(has_up)(lambda: greet((target[UP], tp)))
    pl.when(has_down)(lambda: greet((target[DOWN], tp)))
    greet((target[ACROSS], tp))
    pl.when(has_next)(lambda: greet((sp + 1, tp)))
    pl.when(has_prev)(lambda: greet((sp - 1, tp)))
    for d in range(1, T):
        greet((sp, peer(d)))
    pl.semaphore_wait(
        barrier, T + one(has_up) + one(has_down) + one(has_next) + one(has_prev)
    )

    def remote(p, blk, way):
        return pltpu.make_async_remote_copy(
            src_ref=bufs[p].at[blk],
            dst_ref=bufs[p].at[blk],
            send_sem=send_sem.at[way, p, blk],
            recv_sem=recv_sem.at[p, blk],
            device_id=(target[way], tp),
            device_id_type=MESH,
        )

    def send(p, blk, way, cond=None):
        if cond is None:
            remote(p, blk, way).start()
        else:
            pl.when(cond)(lambda: remote(p, blk, way).start())

    def sent(p, blk, way):
        remote(p, blk, way).wait_send()

    def arrive(p, blk):
        remote(p, blk, ACROSS).wait_recv()

    loads[0].wait()
    send(KV, sp, UP, has_up)
    send(KV, sp, ACROSS, y == 0)
    for p in (UP_B, GATE, UP_A):
        loads[p].wait()
        send(p, sp, DOWN, has_down)
    loads[4].wait()

    m_s[...] = jnp.full(m_s.shape, -1e30, f32)
    l_s[...] = jnp.zeros(l_s.shape, f32)
    acc_s[...] = jnp.zeros(acc_s.shape, f32)
    scale = 1.0 / math.sqrt(dh)

    def attend(blk):
        row_at = sp * rows + lax.broadcasted_iota(jnp.int32, (rows, rows), 0)
        col_at = blk * rows + lax.broadcasted_iota(jnp.int32, (rows, rows), 1)
        keep = col_at <= row_at
        for h in range(heads):
            v = kv[blk, :, 2 * heads * dh + h * dv : 2 * heads * dh + (h + 1) * dv]
            for c in range(2):
                i = 2 * h + c
                k = kv[blk, :, i * dh : (i + 1) * dh]
                s = lax.dot_general(
                    q[:, i * dh : (i + 1) * dh], k, (((1,), (1,)), ((), ())),
                    preferred_element_type=f32,
                ) * scale
                s = jnp.where(keep, s, -1e30)
                old = m_s[i]
                new = jnp.maximum(old, jnp.max(s, axis=1, keepdims=True))
                e = jnp.where(keep, jnp.exp(s - new), 0.0)
                fade = jnp.exp(old - new)
                m_s[i] = new
                l_s[i] = l_s[i] * fade + jnp.sum(e, axis=1, keepdims=True)
                acc_s[i] = acc_s[i] * fade + jnp.dot(e.astype(bf16), v, preferred_element_type=f32)

    @pl.loop(0, Z)
    def _(r):
        @pl.when(z >= r)
        def _():
            blk = sp - 2 * r

            @pl.when(r > 0)
            def _():
                arrive(KV, blk)
                send(KV, blk, UP, has_up)
                send(KV, blk, ACROSS)

            attend(blk)

    for p in (UP_B, GATE, UP_A):
        send(p, sp, ACROSS)
        send(p, sp, UP, has_up)

    @pl.loop(0, Z)
    def _(r):
        @pl.when((z >= r) & ((r > 0) | (y == 1)))
        def _():
            blk = (z - r) * 2 + (1 - y)
            arrive(KV, blk)
            attend(blk)

    def relay(r):
        @pl.when((r == 0))
        def _():
            b = z * 2 + (1 - y)
            arrive(UP_B, b)
            send(UP_B, b, UP, has_up)
            send(UP_B, b, DOWN, has_down)

        def side(exists, col_z, way, cond):
            @pl.when(exists & (r > 0))
            def _():
                a = col_z * 2 + y
                b = col_z * 2 + (1 - y)
                for p in (UP_B, GATE, UP_A):
                    arrive(p, a)
                    send(p, a, way, cond)
                    if p != UP_B:
                        send(p, a, ACROSS)
                    else:
                        pass
                arrive(UP_B, b)
                send(UP_B, b, way, cond)

        side(z + r < Z, z + r, DOWN, has_down)
        side(z >= r, z - r, UP, has_up)

    first = min(2, Z)

    @pl.loop(0, first)
    def _(r):
        relay(r)

    loads[5].wait()
    for h in range(heads):
        a0 = acc_s[2 * h] / l_s[2 * h]
        a1 = acc_s[2 * h + 1] / l_s[2 * h + 1]
        a = a0 - lam_ref[h] * a1
        ms = jnp.mean(a * a, axis=1, keepdims=True)
        n = a * lax.rsqrt(ms + epsilon) * sub_ref[...] * (1.0 - lambda_init)
        n_s[:, h * dv : (h + 1) * dv] = n.astype(bf16)
    width = min(512, D)
    for c in range(0, D, width):
        part[:, :, c : c + width] = (
            jnp.dot(n_s[...], wout[:, c : c + width], preferred_element_type=f32)
            .astype(bf16)
            .reshape(T, own, width)
        )

    def swap(d, src, dst, k):
        return pltpu.make_async_remote_copy(
            src_ref=src, dst_ref=dst, send_sem=tp_send.at[k, d], recv_sem=tp_recv.at[k, d],
            device_id=(sp, peer(d)), device_id_type=MESH,
        )

    firsts = [swap(d, part.at[peer(d)], part_in.at[d], 0) for d in range(1, T)]
    for c in firsts:
        c.start()
    loads[6].wait()
    total = res[pl.ds(tp * own, own), :].astype(f32) + part[tp].astype(f32)
    for d in range(1, T):
        firsts[d - 1].wait_recv()
        total = total + part_in[d].astype(f32)
    mid[...] = total
    ms = jnp.mean(total * total, axis=1, keepdims=True)
    hn[tp] = (total * lax.rsqrt(ms + epsilon) * norm_ref[...]).astype(bf16)
    seconds = [swap(d, hn.at[tp], hn.at[tp], 1) for d in range(1, T)]
    for c in seconds:
        c.start()
    for d in range(1, T):
        back = lax.rem(tp + T - d, T)
        swap(d, hn.at[back], hn.at[back], 1).wait_recv()

    halo = pltpu.make_async_remote_copy(
        src_ref=hn.at[T - 1, pl.ds(own - HALO, HALO)], dst_ref=halo_in,
        send_sem=halo_sem.at[0], recv_sem=halo_sem.at[1],
        device_id=(sp + 1, tp), device_id_type=MESH,
    )
    pl.when(has_next)(halo.start)

    @pl.loop(first, Z)
    def _(r):
        relay(r)

    pl.when(has_prev)(halo.wait_recv)

    @pl.when(jnp.logical_not(has_prev))
    def _():
        halo_in[...] = jnp.zeros(halo_in.shape, bf16)

    for j in range(S):
        hb[j, :HALO, :] = halo_in[:, j * feat : (j + 1) * feat]
        hb[j, HALO:, :] = hn[:, :, j * feat : (j + 1) * feat].reshape(rows, feat)

    acc_g[...] = jnp.zeros(acc_g.shape, f32)
    acc_u[...] = jnp.zeros(acc_u.shape, f32)

    def mul(blk):
        acc_g[...] += jnp.dot(hb[blk], wg[blk], preferred_element_type=f32)
        acc_u[...] += jnp.dot(hb[blk, :, :half], wua[blk], preferred_element_type=f32)
        acc_u[...] += jnp.dot(hb[blk, :, half:], wub[blk], preferred_element_type=f32)

    @pl.loop(0, Z)
    def _(k):
        mul(2 * k + y)

    def take(blk):
        arrive(GATE, blk)
        arrive(UP_A, blk)
        mul(blk)

    @pl.loop(0, Z)
    def _(r):
        pl.when((z + r < Z) & (r > 0))(lambda: take((z + r) * 2 + 1 - y))
        pl.when(z >= r)(lambda: take((z - r) * 2 + 1 - y))

    for c in range(0, units, 128):
        cols = slice(c, c + 128)
        g = acc_g[:, cols].astype(bf16).astype(f32)
        u = acc_u[:, cols].astype(bf16).astype(f32)

        def mix(x, taps):
            out = taps[0:1, cols] * x[HALO - 2 : HALO - 2 + rows]
            out = out + taps[1:2, cols] * x[HALO - 1 : HALO - 1 + rows]
            return out + taps[2:3, cols] * x[HALO:]

        gm, um = mix(g, cg_ref), mix(u, cu_ref)
        hid[:, cols] = (gm / (1.0 + jnp.exp(-gm)) * um).astype(bf16)

    loads[7].wait()
    chunks, cw = low.shape[0], low.shape[3]
    lows = []
    for c in range(chunks):
        low[c] = (
            jnp.dot(hid[...], wd[:, c * cw : (c + 1) * cw], preferred_element_type=f32)
            .astype(bf16)
            .reshape(T, own, cw)
        )
        for d in range(1, T):
            copy = pltpu.make_async_remote_copy(
                src_ref=low.at[c, peer(d)], dst_ref=low_in.at[c, d],
                send_sem=low_send.at[c, d], recv_sem=low_recv.at[c, d],
                device_id=(sp, peer(d)), device_id_type=MESH,
            )
            copy.start()
            lows.append(copy)

    @pl.loop(0, Z)
    def _(k):
        a = 2 * k + y
        b = 2 * k + 1 - y
        pl.when(has_up & (k <= z))(lambda: sent(KV, a, UP))
        pl.when((k < z) | ((k == z) & (y == 0)))(lambda: sent(KV, a, ACROSS))
        for p in (GATE, UP_A):
            sent(p, a, ACROSS)
        pl.when(k == z)(lambda: sent(UP_B, a, ACROSS))
        for p, blk in ((GATE, a), (UP_A, a), (UP_B, a), (UP_B, b)):
            pl.when(has_up & (k <= z))(functools.partial(sent, p, blk, UP))
            pl.when(has_down & (k >= z))(functools.partial(sent, p, blk, DOWN))

    for c in firsts + seconds:
        c.wait_send()
    pl.when(has_next)(halo.wait_send)

    for c in range(chunks):
        cols = slice(c * cw, (c + 1) * cw)
        total = mid[:, cols] + low[c, tp].astype(f32)
        for d in range(1, T):
            lows[c * (T - 1) + d - 1].wait_recv()
            total = total + low_in[c, d].astype(f32)
        out_ref[:, cols] = total.astype(bf16)
    for c in lows:
        c.wait_send()


def local(
    S, T,
    residual, queries, key_rows, values, lambda_head, sub_gain, w_out, norm_gain,
    w_gate, w_up, conv_gate, conv_up, w_down,
):
    rows, heads, maps, dh = queries.shape
    dv = values.shape[2]
    feat, units = w_gate.shape
    D = w_out.shape[1]
    own = rows // T
    half = feat // 2
    q = queries.reshape(rows, heads * maps * dh)
    kv = jnp.concatenate(
        [key_rows.reshape(rows, heads * maps * dh), values.reshape(rows, heads * dv)], axis=1
    )
    kvw = kv.shape[1]
    cw = math.gcd(D, 512)
    chunks = D // cw
    hbm = pl.BlockSpec(memory_space=pl.ANY)
    vmem = pl.BlockSpec(memory_space=pltpu.VMEM)
    smem = pl.BlockSpec(memory_space=pltpu.SMEM)
    padded = rows + HALO
    V = pltpu.VMEM
    dma = pltpu.SemaphoreType.DMA
    return pl.pallas_call(
        functools.partial(kernel, S, T, heads, dh, dv),
        out_shape=jax.ShapeDtypeStruct((own, D), bf16),
        in_specs=[hbm] * 7 + [smem] + [vmem] * 4,
        out_specs=vmem,
        scratch_shapes=[
            V((rows, q.shape[1]), bf16),
            V((S, rows, kvw), bf16),
            V((rows, D), bf16),
            V(w_out.shape, bf16),
            V((S, feat, units), bf16),
            V((S, half, units), bf16),
            V((S, half, units), bf16),
            V(w_down.shape, bf16),
            V((2 * heads, rows, 1), f32),
            V((2 * heads, rows, 1), f32),
            V((2 * heads, rows, dv), f32),
            V((rows, heads * dv), bf16),
            V((T, own, D), bf16),
            V((T, own, D), bf16),
            V((own, D), f32),
            V((T, own, D), bf16),
            V((S, padded, feat), bf16),
            V((HALO, D), bf16),
            V((padded, units), f32),
            V((padded, units), f32),
            V((rows, units), bf16),
            V((chunks, T, own, cw), bf16),
            V((chunks, T, own, cw), bf16),
            dma((8,)),
            dma((3, 4, S)),
            dma((4, S)),
            dma((2, T)),
            dma((2, T)),
            dma((2,)),
            dma((chunks, T)),
            dma((chunks, T)),
        ],
        compiler_params=pltpu.CompilerParams(
            collective_id=0, has_side_effects=True, vmem_limit_bytes=64000000
        ),
    )(
        q, kv, residual, w_out, w_gate, w_up, w_down, lambda_head,
        sub_gain.reshape(1, -1), norm_gain.reshape(1, -1), conv_gate, conv_up,
    )


def solution(mesh):
    placed = (
        P("sp", None),
        P("sp", "tp", None, None),
        P("sp", "tp", None, None),
        P("sp", "tp", None),
        P("tp"),
        P(),
        P("tp", None),
        P(),
        P("sp", "tp"),
        P("sp", "tp"),
        P(None, "tp"),
        P(None, "tp"),
        P("tp", None),
    )
    return jax.shard_map(
        functools.partial(local, mesh.shape["sp"], mesh.shape["tp"]),
        mesh=mesh, in_specs=placed, out_specs=P(("sp", "tp"), None), check_vma=False,
    )
```

```python
import functools
import math

import jax
import jax.numpy as jnp
from jax import lax
from jax.experimental import pallas as pl
from jax.experimental.pallas import tpu as pltpu
from jax.sharding import PartitionSpec as P

MESH = pl.DeviceIdType.MESH
epsilon = 1e-06
lambda_init = 0.8 - 0.6 * math.exp(-0.3)
bf16 = jnp.bfloat16
f32 = jnp.float32
HALO = 16
UP, DOWN, ACROSS = 0, 1, 2
KV, GATE, UP_A, UP_B = 0, 1, 2, 3


def kernel(
    S, T, heads, dh, dv,
    q_hbm, kv_hbm, res_hbm, wout_hbm, wg_hbm, wu_hbm, wd_hbm,
    lam_ref, sub_ref, norm_ref, cg_ref, cu_ref,
    out_ref,
    q, kv, res, wout, wg, wua, wub, wd,
    m_s, l_s, acc_s, n_own, n_in, part, part_in, mid, hn, hb, halo_in, acc_g, acc_u, hid, low, low_in,
    local_sem, pair_sem, send_sem, recv_sem, tp_send, tp_recv, halo_sem, low_send, low_recv,
):
    Z = S // 2
    sp = lax.axis_index("sp")
    tp = lax.axis_index("tp")
    z = lax.div(sp, 2)
    y = lax.rem(sp, 2)
    rows = q.shape[1]
    feat = wg.shape[1]
    tail = wub.shape[2]
    split = wua.shape[2]
    hh = heads // 2
    kw = 2 * hh * dh
    D = wout.shape[1]
    own = rows // T
    units = wg.shape[2]
    has_up, has_down = z < Z - 1, z > 0
    has_next, has_prev = sp < S - 1, sp > 0

    def one(flag):
        return flag.astype(jnp.int32)

    def peer(d):
        return lax.rem(tp + d, T)

    target = {UP: sp + 2, DOWN: sp - 2, ACROSS: z * 2 + (1 - y)}
    bufs = {KV: kv, GATE: wg, UP_A: wua, UP_B: wub}

    loads = [
        pltpu.make_async_copy(kv_hbm.at[y], kv.at[sp], local_sem.at[0]),
        pltpu.make_async_copy(wg_hbm, wg.at[sp], local_sem.at[1]),
        pltpu.make_async_copy(wu_hbm.at[:, pl.ds(0, split)], wua.at[sp], local_sem.at[2]),
        pltpu.make_async_copy(wu_hbm.at[:, pl.ds(split, tail)], wub.at[sp], local_sem.at[3]),
        pltpu.make_async_copy(q_hbm.at[y], q.at[y], local_sem.at[4]),
        pltpu.make_async_copy(wout_hbm, wout, local_sem.at[5]),
        pltpu.make_async_copy(res_hbm, res, local_sem.at[6]),
        pltpu.make_async_copy(wd_hbm, wd, local_sem.at[7]),
    ]
    for c in loads:
        c.start()

    barrier = pltpu.get_barrier_semaphore()

    def greet(device):
        pl.semaphore_signal(barrier, inc=1, device_id=device, device_id_type=MESH)

    pl.when(has_up)(lambda: greet((target[UP], tp)))
    pl.when(has_down)(lambda: greet((target[DOWN], tp)))
    greet((target[ACROSS], tp))
    pl.when(has_next)(lambda: greet((sp + 1, tp)))
    pl.when(has_prev)(lambda: greet((sp - 1, tp)))
    for d in range(1, T):
        greet((sp, peer(d)))
    pl.semaphore_wait(
        barrier, T + one(has_up) + one(has_down) + one(has_next) + one(has_prev)
    )

    def remote(p, blk, way):
        return pltpu.make_async_remote_copy(
            src_ref=bufs[p].at[blk],
            dst_ref=bufs[p].at[blk],
            send_sem=send_sem.at[way, p, blk],
            recv_sem=recv_sem.at[p, blk],
            device_id=(target[way], tp),
            device_id_type=MESH,
        )

    def send(p, blk, way, cond=None):
        if cond is None:
            remote(p, blk, way).start()
        else:
            pl.when(cond)(lambda: remote(p, blk, way).start())

    def sent(p, blk, way):
        remote(p, blk, way).wait_send()

    def arrive(p, blk):
        remote(p, blk, ACROSS).wait_recv()

    other = 1 - y
    across = (target[ACROSS], tp)

    def pair(src, dst, k):
        return pltpu.make_async_remote_copy(
            src_ref=src, dst_ref=dst, send_sem=pair_sem.at[0, k], recv_sem=pair_sem.at[1, k],
            device_id=across, device_id_type=MESH,
        )

    kv_swap = pair(kv_hbm.at[other], kv.at[sp], 0)
    q_swap = pair(q_hbm.at[other], q.at[y], 1)
    kv_got = pair(kv_hbm.at[other], kv.at[target[ACROSS]], 0)
    q_got = pair(q_hbm.at[other], q.at[other], 1)
    kv_swap.start()
    q_swap.start()
    loads[0].wait()
    send(KV, sp, UP, has_up)
    for p in (UP_B, GATE, UP_A):
        loads[p].wait()
        send(p, sp, DOWN, has_down)
        send(p, sp, ACROSS)
    loads[4].wait()

    m_s[...] = jnp.full(m_s.shape, -1e30, f32)
    l_s[...] = jnp.zeros(l_s.shape, f32)
    acc_s[...] = jnp.zeros(acc_s.shape, f32)
    scale = 1.0 / math.sqrt(dh)

    def attend(yy, blk):
        row_at = (z * 2 + yy) * rows + lax.broadcasted_iota(jnp.int32, (rows, rows), 0)
        col_at = blk * rows + lax.broadcasted_iota(jnp.int32, (rows, rows), 1)
        keep = col_at <= row_at
        for h in range(hh):
            v = kv[blk, :, kw + h * dv : kw + (h + 1) * dv]
            for c in range(2):
                i = 2 * h + c
                k = kv[blk, :, i * dh : (i + 1) * dh]
                s = lax.dot_general(
                    q[yy, :, i * dh : (i + 1) * dh], k, (((1,), (1,)), ((), ())),
                    preferred_element_type=f32,
                ) * scale
                s = jnp.where(keep, s, -1e30)
                old = m_s[yy, i]
                new = jnp.maximum(old, jnp.max(s, axis=1, keepdims=True))
                e = jnp.where(keep, jnp.exp(s - new), 0.0)
                fade = jnp.exp(old - new)
                m_s[yy, i] = new
                l_s[yy, i] = l_s[yy, i] * fade + jnp.sum(e, axis=1, keepdims=True)
                acc_s[yy, i] = acc_s[yy, i] * fade + jnp.dot(
                    e.astype(bf16), v, preferred_element_type=f32
                )

    kv_got.wait_recv()
    q_got.wait_recv()
    send(KV, target[ACROSS], UP, has_up)

    @pl.loop(0, Z)
    def _(r):
        @pl.when(z >= r)
        def _():
            @pl.when(r > 0)
            def _():
                for blk in (sp - 2 * r, target[ACROSS] - 2 * r):
                    arrive(KV, blk)
                    send(KV, blk, UP, has_up)

            @pl.loop(0, 4)
            def _(i):
                yy, c = lax.div(i, 2), lax.rem(i, 2)
                pl.when((r > 0) | (yy >= c))(lambda: attend(yy, (z - r) * 2 + c))

    for p in (UP_B, GATE, UP_A):
        send(p, sp, UP, has_up)

    for yy in range(2):
        for h in range(hh):
            a0 = acc_s[yy, 2 * h] / l_s[yy, 2 * h]
            a1 = acc_s[yy, 2 * h + 1] / l_s[yy, 2 * h + 1]
            a = a0 - lam_ref[y * hh + h] * a1
            ms = jnp.mean(a * a, axis=1, keepdims=True)
            n = a * lax.rsqrt(ms + epsilon) * sub_ref[...] * (1.0 - lambda_init)
            n_own[yy, :, h * dv : (h + 1) * dv] = n.astype(bf16)
    n_swap = pair(n_own.at[other], n_in, 2)
    n_swap.start()

    def relay(r):
        @pl.when((r == 0))
        def _():
            b = z * 2 + (1 - y)
            arrive(UP_B, b)
            send(UP_B, b, UP, has_up)
            send(UP_B, b, DOWN, has_down)

        def side(exists, col_z, way, cond):
            @pl.when(exists & (r > 0))
            def _():
                a = col_z * 2 + y
                b = col_z * 2 + (1 - y)
                for p in (GATE, UP_A, UP_B):
                    arrive(p, a)
                    send(p, a, way, cond)
                    if p != UP_B:
                        send(p, a, ACROSS)
                arrive(UP_B, b)
                send(UP_B, b, way, cond)

        side(z + r < Z, z + r, DOWN, has_down)
        side(z >= r, z - r, UP, has_up)

    first = min(2, Z)

    @pl.loop(0, first)
    def _(r):
        relay(r)

    loads[5].wait()
    n_swap.wait_recv()
    width = min(512, D)
    hw = hh * dv
    for c in range(0, D, width):
        cols = slice(c, c + width)
        part[:, :, cols] = (
            (
                jnp.dot(n_own[y], wout[pl.ds(y * hw, hw), cols], preferred_element_type=f32)
                + jnp.dot(n_in[...], wout[pl.ds(other * hw, hw), cols], preferred_element_type=f32)
            )
            .astype(bf16)
            .reshape(T, own, width)
        )

    def swap(d, src, dst, k):
        return pltpu.make_async_remote_copy(
            src_ref=src, dst_ref=dst, send_sem=tp_send.at[k, d], recv_sem=tp_recv.at[k, d],
            device_id=(sp, peer(d)), device_id_type=MESH,
        )

    firsts = [swap(d, part.at[peer(d)], part_in.at[d], 0) for d in range(1, T)]
    for c in firsts:
        c.start()
    loads[6].wait()
    total = res[pl.ds(tp * own, own), :].astype(f32) + part[tp].astype(f32)
    for d in range(1, T):
        firsts[d - 1].wait_recv()
        total = total + part_in[d].astype(f32)
    mid[...] = total
    ms = jnp.mean(total * total, axis=1, keepdims=True)
    hn[tp] = (total * lax.rsqrt(ms + epsilon) * norm_ref[...]).astype(bf16)
    seconds = [swap(d, hn.at[tp], hn.at[tp], 1) for d in range(1, T)]
    for c in seconds:
        c.start()
    for d in range(1, T):
        back = lax.rem(tp + T - d, T)
        swap(d, hn.at[back], hn.at[back], 1).wait_recv()

    halo = pltpu.make_async_remote_copy(
        src_ref=hn.at[T - 1, pl.ds(own - HALO, HALO)], dst_ref=halo_in,
        send_sem=halo_sem.at[0], recv_sem=halo_sem.at[1],
        device_id=(sp + 1, tp), device_id_type=MESH,
    )
    pl.when(has_next)(halo.start)

    @pl.loop(first, Z)
    def _(r):
        relay(r)

    pl.when(has_prev)(halo.wait_recv)

    @pl.when(jnp.logical_not(has_prev))
    def _():
        halo_in[...] = jnp.zeros(halo_in.shape, bf16)

    for j in range(S):
        hb[j, :HALO, :] = halo_in[:, j * feat : (j + 1) * feat]
        hb[j, HALO:, :] = hn[:, :, j * feat : (j + 1) * feat].reshape(rows, feat)

    acc_g[...] = jnp.zeros(acc_g.shape, f32)
    acc_u[...] = jnp.zeros(acc_u.shape, f32)

    def mul(blk):
        acc_g[...] += jnp.dot(hb[blk], wg[blk], preferred_element_type=f32)
        acc_u[:, :split] += jnp.dot(hb[blk], wua[blk], preferred_element_type=f32)
        acc_u[:, split:] += jnp.dot(hb[blk], wub[blk], preferred_element_type=f32)

    @pl.loop(0, Z)
    def _(k):
        mul(2 * k + y)

    def take(blk):
        arrive(GATE, blk)
        arrive(UP_A, blk)
        mul(blk)

    @pl.loop(0, Z)
    def _(r):
        pl.when((z + r < Z) & (r > 0))(lambda: take((z + r) * 2 + 1 - y))
        pl.when(z >= r)(lambda: take((z - r) * 2 + 1 - y))

    for c in range(0, units, 128):
        cols = slice(c, c + 128)
        g = acc_g[:, cols].astype(bf16).astype(f32)
        u = acc_u[:, cols].astype(bf16).astype(f32)

        def mix(x, taps):
            out = taps[0:1, cols] * x[HALO - 2 : HALO - 2 + rows]
            out = out + taps[1:2, cols] * x[HALO - 1 : HALO - 1 + rows]
            return out + taps[2:3, cols] * x[HALO:]

        gm, um = mix(g, cg_ref), mix(u, cu_ref)
        hid[:, cols] = (gm / (1.0 + jnp.exp(-gm)) * um).astype(bf16)

    loads[7].wait()
    chunks, cw = low.shape[0], low.shape[3]
    lows = []
    for c in range(chunks):
        low[c] = (
            jnp.dot(hid[...], wd[:, c * cw : (c + 1) * cw], preferred_element_type=f32)
            .astype(bf16)
            .reshape(T, own, cw)
        )
        for d in range(1, T):
            copy = pltpu.make_async_remote_copy(
                src_ref=low.at[c, peer(d)], dst_ref=low_in.at[c, d],
                send_sem=low_send.at[c, d], recv_sem=low_recv.at[c, d],
                device_id=(sp, peer(d)), device_id_type=MESH,
            )
            copy.start()
            lows.append(copy)

    @pl.loop(0, Z)
    def _(k):
        a = 2 * k + y
        b = 2 * k + 1 - y
        for p in (GATE, UP_A):
            sent(p, a, ACROSS)
        pl.when(k == z)(lambda: sent(UP_B, a, ACROSS))
        for p, blk in ((KV, a), (KV, b), (GATE, a), (UP_A, a), (UP_B, a), (UP_B, b)):
            pl.when(has_up & (k <= z))(functools.partial(sent, p, blk, UP))
            if p != KV:
                pl.when(has_down & (k >= z))(functools.partial(sent, p, blk, DOWN))

    for c in firsts + seconds + [kv_swap, q_swap, n_swap]:
        c.wait_send()
    pl.when(has_next)(halo.wait_send)

    for c in range(chunks):
        cols = slice(c * cw, (c + 1) * cw)
        total = mid[:, cols] + low[c, tp].astype(f32)
        for d in range(1, T):
            lows[c * (T - 1) + d - 1].wait_recv()
            total = total + low_in[c, d].astype(f32)
        out_ref[:, cols] = total.astype(bf16)
    for c in lows:
        c.wait_send()


def local(
    S, T,
    residual, queries, key_rows, values, lambda_head, sub_gain, w_out, norm_gain,
    w_gate, w_up, conv_gate, conv_up, w_down,
):
    rows, heads, maps, dh = queries.shape
    dv = values.shape[2]
    feat, units = w_gate.shape
    D = w_out.shape[1]
    own = rows // T
    tail = 3 * math.gcd(units, 128)
    hh = heads // 2
    q = queries.reshape(rows, 2, hh * maps * dh).swapaxes(0, 1)
    kv = jnp.concatenate(
        [key_rows.reshape(rows, 2, hh * maps * dh), values.reshape(rows, 2, hh * dv)], axis=2
    ).swapaxes(0, 1)
    kvw = kv.shape[2]
    cw = math.gcd(D, 512)
    chunks = D // cw
    hbm = pl.BlockSpec(memory_space=pl.ANY)
    vmem = pl.BlockSpec(memory_space=pltpu.VMEM)
    smem = pl.BlockSpec(memory_space=pltpu.SMEM)
    padded = rows + HALO
    V = pltpu.VMEM
    dma = pltpu.SemaphoreType.DMA
    return pl.pallas_call(
        functools.partial(kernel, S, T, heads, dh, dv),
        out_shape=jax.ShapeDtypeStruct((own, D), bf16),
        in_specs=[hbm] * 7 + [smem] + [vmem] * 4,
        out_specs=vmem,
        scratch_shapes=[
            V(q.shape, bf16),
            V((S, rows, kvw), bf16),
            V((rows, D), bf16),
            V(w_out.shape, bf16),
            V((S, feat, units), bf16),
            V((S, feat, units - tail), bf16),
            V((S, feat, tail), bf16),
            V(w_down.shape, bf16),
            V((2, 2 * hh, rows, 1), f32),
            V((2, 2 * hh, rows, 1), f32),
            V((2, 2 * hh, rows, dv), f32),
            V((2, rows, hh * dv), bf16),
            V((rows, hh * dv), bf16),
            V((T, own, D), bf16),
            V((T, own, D), bf16),
            V((own, D), f32),
            V((T, own, D), bf16),
            V((S, padded, feat), bf16),
            V((HALO, D), bf16),
            V((padded, units), f32),
            V((padded, units), f32),
            V((rows, units), bf16),
            V((chunks, T, own, cw), bf16),
            V((chunks, T, own, cw), bf16),
            dma((8,)),
            dma((2, 3)),
            dma((3, 4, S)),
            dma((4, S)),
            dma((2, T)),
            dma((2, T)),
            dma((2,)),
            dma((chunks, T)),
            dma((chunks, T)),
        ],
        compiler_params=pltpu.CompilerParams(
            collective_id=0, has_side_effects=True, vmem_limit_bytes=64000000
        ),
    )(
        q, kv, residual, w_out, w_gate, w_up, w_down, lambda_head,
        sub_gain.reshape(1, -1), norm_gain.reshape(1, -1), conv_gate, conv_up,
    )


def solution(mesh):
    placed = (
        P("sp", None),
        P("sp", "tp", None, None),
        P("sp", "tp", None, None),
        P("sp", "tp", None),
        P("tp"),
        P(),
        P("tp", None),
        P(),
        P("sp", "tp"),
        P("sp", "tp"),
        P(None, "tp"),
        P(None, "tp"),
        P("tp", None),
    )
    return jax.shard_map(
        functools.partial(local, mesh.shape["sp"], mesh.shape["tp"]),
        mesh=mesh, in_specs=placed, out_specs=P(("sp", "tp"), None), check_vma=False,
    )
```
